32 devices in a mesh: sp: 8 (over z, y), tp: 4 (over x, core).
Axes of the slice: x: 2, y: 2, z: 4, core: 2. Of those that a mesh axis runs over, the one named last changes fastest.
Arguments:
- activity: bfloat16 [2048, 4096], P('sp', 'tp'), may hold values from -8 to 8
- query_weight: bfloat16 [4096, 3072], P('sp', 'tp'), may hold values from -0.09375 to 0.09375
- key_weight: bfloat16 [4096, 3072], P('sp', 'tp'), may hold values from -0.09375 to 0.09375
- value_weight: bfloat16 [4096, 3072], P('sp', 'tp'), may hold values from -0.09375 to 0.09375
- merge_weight: bfloat16 [1024, 4096], P('tp', 'sp'), may hold values from -1.5 to 1.5
Outputs:
- attended: bfloat16 [2048, 4096], P(('sp', 'tp'))
The draws below stay inside these ranges and needn't reach their ends.
All inputs are finite; a program needn't handle non-finite values.
Results may differ from the reference program's by a relative error of at most 0.013.
Values may be sent and summed in bfloat16 or wider, within the bound.
A program may use at most 128 MiB of HBM per device.

```python
import jax
import jax.numpy as jnp
from jax import lax

D = 4096
HPG = 16
HEAD = 64
HEAD_GROUPS = 3
SPAN = 128
DILATION_MIDDLE = 4
DILATION_WIDEST = 8
TOK_DEV = 256
TOKENS = 2048


def draw_activity(key, part):
    key_base, key_sign = jax.random.split(key, 2)
    drawn = jnp.clip(jax.random.normal(key_base, (TOKENS, D), jnp.float32), -6.0, 6.0)
    return drawn.astype(jnp.bfloat16)


def paired_weights(key):
    key_query = jax.random.fold_in(key, 11)
    key_other = jax.random.fold_in(key, 23)
    col_total = HEAD_GROUPS * HPG * HEAD
    weight_scale = D ** (-0.5)
    query_draw = jnp.clip(jax.random.normal(key_query, (D, col_total), jnp.float32), -6.0, 6.0) * weight_scale
    key_draw = jnp.clip(jax.random.normal(key_other, (D, col_total), jnp.float32), -6.0, 6.0) * weight_scale
    return (query_draw, key_draw)


def draw_query_weight(key, part):
    return paired_weights(key)[0].astype(jnp.bfloat16)


def draw_key_weight(key, part):
    return paired_weights(key)[1].astype(jnp.bfloat16)


def shard_levels(stream_key, extent, cuts, smallest, largest):
    def one(position, parts):
        heights = jax.random.uniform(jax.random.fold_in(jax.random.fold_in(stream_key, 6), position), (parts,), jnp.float32, smallest / len(cuts), largest / len(cuts))
        return jnp.repeat(jnp.exp(heights), extent[position] // parts).reshape((-1,) + (1,) * (len(extent) - position - 1))

    gain = one(*cuts[0])
    for cut in cuts[1:]:
        gain = gain * one(*cut)
    return gain


def noise(key, shape, width, reach, pieces=(), kind=jnp.bfloat16):
    values = jax.random.normal(key, shape, jnp.float32) * width
    if len(pieces) > 0:
        values = shard_levels(key, shape, pieces, -0.22, 0.18) * values
    return jnp.clip(values, min=-reach, max=reach).astype(kind)


def setup_inputs(seed: int = 0) -> dict:
    splits = jax.random.split(jax.random.key(seed), 6)
    activity = draw_activity(jax.random.fold_in(splits[5], 71), 0)
    query_weight = draw_query_weight(jax.random.fold_in(splits[5], 71), 0)
    key_weight = draw_key_weight(jax.random.fold_in(splits[5], 71), 0)
    value_weight = noise(splits[3], (D, HEAD_GROUPS * HPG * HEAD), D ** -0.5, 0.09375, ((0, 8), (1, 4)))
    merge_weight = noise(splits[4], (HPG * HEAD, D), (HEAD // 4) ** -0.5, 1.5, ((0, 4), (1, 8)))
    return dict(activity=activity, query_weight=query_weight, key_weight=key_weight, value_weight=value_weight, merge_weight=merge_weight)


rope_base = 500000.0


def rotate(channels, angle_pos):
    half_width = channels.shape[-1] // 2
    frequency = rope_base ** (-jnp.arange(0, half_width, dtype=jnp.float32) * 2.0 / channels.shape[-1])
    angles = angle_pos[:, None] * frequency[None, :]
    cosine = jnp.cos(angles)[:, None, None, :]
    sine_part = jnp.sin(angles)[:, None, None, :]
    first_half = channels[..., :half_width]
    second_half = channels[..., half_width:]
    return jnp.concatenate([first_half * cosine - second_half * sine_part, second_half * cosine + first_half * sine_part], axis=-1)


def window_mix(queries, key_rows, value_entries, query_pos, key_pos, dilation, reach_rows):
    scores = jnp.einsum('ahc,rhc->har', queries.astype(jnp.float32), key_rows.astype(jnp.float32)) * (queries.shape[-1] ** -0.5)
    distance = query_pos[:, None] - key_pos[None, :]
    allowed = (distance >= 0) & (distance <= reach_rows) & (distance % dilation == 0) & (key_pos[None, :] >= 0)
    scores = jnp.where(allowed[None], scores, -jnp.inf)
    row_max = jnp.max(scores, axis=-1, keepdims=True)
    expo = jnp.where(allowed[None], jnp.exp(scores - row_max), 0.0)
    denominator = jnp.sum(expo, axis=-1)
    rounded = lax.optimization_barrier(expo.astype(jnp.bfloat16)).astype(jnp.float32)
    mixed = jnp.einsum('har,rhc->ahc', rounded, value_entries.astype(jnp.float32))
    mixed = mixed / jnp.transpose(denominator)[:, :, None]
    log_total = jnp.transpose(row_max[..., 0] + jnp.log(denominator))
    return mixed, log_total


def reference(activity, query_weight, key_weight, value_weight, merge_weight):
    tok_total = activity.shape[0]
    local_heads = query_weight.shape[1] // (HEAD_GROUPS * HEAD)
    angle_pos = jnp.arange(tok_total, dtype=jnp.int32).astype(jnp.float32)

    def project(weight):
        return jnp.dot(activity, weight, preferred_element_type=jnp.float32).reshape(tok_total, local_heads, HEAD_GROUPS, HEAD)

    query_all = lax.optimization_barrier(rotate(project(query_weight), angle_pos).astype(jnp.bfloat16))
    key_all = lax.optimization_barrier(rotate(project(key_weight), angle_pos).astype(jnp.bfloat16))
    value_all = lax.optimization_barrier(project(value_weight).astype(jnp.bfloat16))
    group_dilations = (1, DILATION_MIDDLE, DILATION_WIDEST)
    query_groups = []
    padded = []
    for grp_index in range(HEAD_GROUPS):
        reach_rows = SPAN * group_dilations[grp_index]
        query_groups.append(query_all[:, :, grp_index])
        padded.append((jnp.pad(key_all[:, :, grp_index], ((reach_rows, 0), (0, 0), (0, 0))),
                       jnp.pad(value_all[:, :, grp_index], ((reach_rows, 0), (0, 0), (0, 0)))))

    def one_block(block_index):
        start_row = block_index * TOK_DEV
        query_pos = start_row + jnp.arange(TOK_DEV, dtype=jnp.int32)
        mixed_list = []
        total_list = []
        for grp_index in range(HEAD_GROUPS):
            dilation = group_dilations[grp_index]
            reach_rows = SPAN * dilation
            query_blk = lax.dynamic_slice_in_dim(query_groups[grp_index], start_row, TOK_DEV, 0)
            key_blk = lax.dynamic_slice_in_dim(padded[grp_index][0], start_row, reach_rows + TOK_DEV, 0)
            value_blk = lax.dynamic_slice_in_dim(padded[grp_index][1], start_row, reach_rows + TOK_DEV, 0)
            key_pos = start_row - reach_rows + jnp.arange(reach_rows + TOK_DEV, dtype=jnp.int32)
            mixed, log_total = window_mix(query_blk, key_blk, value_blk, query_pos, key_pos, dilation, reach_rows)
            mixed_list.append(mixed)
            total_list.append(log_total)
        total_stack = jnp.stack(total_list)
        peak_total = jnp.max(total_stack, axis=0)
        shifted = jnp.exp(total_stack - peak_total)
        group_weight = shifted / jnp.sum(shifted, axis=0)
        merged = jnp.sum(group_weight[..., None] * jnp.stack(mixed_list), axis=0)
        return merged.astype(jnp.bfloat16).reshape(TOK_DEV, local_heads * HEAD)

    merged_all = lax.map(one_block, jnp.arange(tok_total // TOK_DEV, dtype=jnp.int32))
    merged_all = merged_all.reshape(tok_total, local_heads * HEAD)
    return jnp.dot(merged_all, merge_weight, preferred_element_type=jnp.float32).astype(jnp.bfloat16)
```

```python
import functools

import jax
import jax.numpy as jnp
from jax import lax
from jax.experimental import pallas as pl
from jax.experimental.pallas import tpu as pltpu
from jax.sharding import PartitionSpec as P

HEAD = 64
HEAD_GROUPS = 3
SPAN = 128
DILATIONS = (1, 4, 8)
MESH = pl.DeviceIdType.MESH

rope_base = 500000.0


def project_kernel(
    G, R, act, wq, wk, wv, out,
    a_buf, w_buf, c_buf, r_buf,
    local_sem, swap_send, swap_recv, fan_send, fan_recv,
    w_send, w_recv, c_send, c_recv,
):
    s = lax.axis_index("sp")
    t = lax.axis_index("tp")
    g = lax.div(s, R)
    r = lax.rem(s, R)
    tok = act.shape[0]
    krows = wq.shape[0]
    width = wq.shape[1] // G
    pairs = G // 2
    weights = (wq, wk, wv)

    swap_dev = (t * R + r, g)
    barrier = pltpu.get_barrier_semaphore()

    def greet(dev):
        pl.semaphore_signal(barrier, inc=1, device_id=dev, device_id_type=MESH)

    for i in range(1, G):
        greet((s, lax.rem(t + i, G)))
        greet((lax.rem(g + i, G) * R + r, t))
    for i in range(1, R):
        greet((g * R + lax.rem(r + i, R), t))

    @pl.when(g != t)
    def _():
        greet(swap_dev)

    pl.semaphore_wait(barrier, 2 * (G - 1) + (R - 1) + jnp.where(g != t, 1, 0))

    def swap_copy():
        return pltpu.make_async_remote_copy(
            src_ref=act, dst_ref=a_buf.at[g], send_sem=swap_send, recv_sem=swap_recv,
            device_id=swap_dev, device_id_type=MESH)

    def swap_local():
        return pltpu.make_async_copy(act, a_buf.at[t], local_sem)

    @pl.when(g != t)
    def _():
        swap_copy().start()

    @pl.when(g == t)
    def _():
        swap_local().start()

    def pair_at(stage):
        return lax.rem(lax.div(g, 2) + 1 + stage, pairs)

    def pair_cols(stage):
        return pl.ds(pl.multiple_of(pair_at(stage) * (2 * width), 128), 2 * width)

    def w_copy(stage, i, x):
        cols = pair_cols(stage)
        return pltpu.make_async_remote_copy(
            src_ref=weights[x].at[:, cols], dst_ref=w_buf.at[i - 1, x, :, cols],
            send_sem=w_send.at[stage, i - 1, x], recv_sem=w_recv.at[stage, i - 1, x],
            device_id=(g * R + lax.rem(r + R - i, R), t), device_id_type=MESH)

    for stage in range(pairs):
        for i in range(1, R):
            for x in range(3):
                w_copy(stage, i, x).start()

    @pl.when(g != t)
    def _():
        swap_copy().wait_recv()

    @pl.when(g == t)
    def _():
        swap_local().wait()

    def fan_copy(i):
        return pltpu.make_async_remote_copy(
            src_ref=a_buf.at[t], dst_ref=a_buf.at[t], send_sem=fan_send.at[i - 1],
            recv_sem=fan_recv.at[i - 1],
            device_id=(s, lax.rem(t + i, G)), device_id_type=MESH)

    def fan_arrival(i):
        slot = lax.rem(t + G - i, G)
        return pltpu.make_async_remote_copy(
            src_ref=a_buf.at[slot], dst_ref=a_buf.at[slot], send_sem=fan_send.at[i - 1],
            recv_sem=fan_recv.at[i - 1],
            device_id=(s, lax.rem(t + i, G)), device_id_type=MESH)

    for i in range(1, G):
        fan_copy(i).start()
    for i in range(1, G):
        fan_arrival(i).wait_recv()

    def c_copy(stage, j, b):
        dest = pair_at(stage) * 2 + j
        rows = pl.ds(pl.multiple_of(b * tok, tok), tok)
        return pltpu.make_async_remote_copy(
            src_ref=c_buf.at[stage, j, rows], dst_ref=r_buf.at[g, rows],
            send_sem=c_send.at[stage, j, b], recv_sem=c_recv.at[g, b],
            device_id=(dest * R + r, t), device_id_type=MESH)

    for stage in range(pairs):
        for i in range(1, R):
            for x in range(3):
                w_copy(stage, i, x).wait_recv()
        cols = pair_cols(stage)

        @pl.loop(0, G)
        def _(b):
            parts = []
            for x in range(3):
                total = jnp.dot(
                    a_buf[b, :, pl.ds(pl.multiple_of(r * krows, 128), krows)],
                    weights[x][:, cols], preferred_element_type=jnp.float32)
                for i in range(1, R):
                    start = pl.multiple_of(lax.rem(r + i, R) * krows, 128)
                    total = total + jnp.dot(
                        a_buf[b, :, pl.ds(start, krows)], w_buf[i - 1, x, :, cols],
                        preferred_element_type=jnp.float32)
                parts.append(total)
            rows = pl.ds(pl.multiple_of(b * tok, tok), tok)
            for j in range(2):
                c_buf[stage, j, rows, :] = jnp.concatenate(
                    [part[:, j * width:(j + 1) * width] for part in parts], axis=1
                ).astype(jnp.bfloat16)
            for j in range(2):
                @pl.when(pair_at(stage) * 2 + j != g)
                def _():
                    c_copy(stage, j, b).start()

    def c_arrival(source, b):
        rows = pl.ds(pl.multiple_of(b * tok, tok), tok)
        return pltpu.make_async_remote_copy(
            src_ref=r_buf.at[source, rows], dst_ref=r_buf.at[source, rows],
            send_sem=c_send.at[0, 0, b], recv_sem=c_recv.at[source, b],
            device_id=(s, t), device_id_type=MESH)

    mine = lax.rem(g, 2)

    @pl.loop(0, G)
    def _(b):
        rows = pl.ds(pl.multiple_of(b * tok, tok), tok)
        total = c_buf[pairs - 1, mine, rows, :].astype(jnp.float32)
        for i in range(1, G):
            source = lax.rem(g + i, G)
            c_arrival(source, b).wait_recv()
            total = total + r_buf[source, rows, :].astype(jnp.float32)
        out[rows, :] = total

    @pl.when(g != t)
    def _():
        swap_copy().wait_send()

    for i in range(1, G):
        fan_copy(i).wait_send()
    for stage in range(pairs):
        for i in range(1, R):
            for x in range(3):
                w_copy(stage, i, x).wait_send()
        for j in range(2):
            @pl.when(pair_at(stage) * 2 + j != g)
            def _():
                @pl.loop(0, G)
                def _(b):
                    c_copy(stage, j, b).wait_send()


def project(activity, wq, wk, wv, G, R):
    tok, feat = activity.shape
    krows, col_width = wq.shape
    width = 3 * (col_width // G)
    pairs = G // 2
    rows = G * tok
    dma = pltpu.SemaphoreType.DMA
    return pl.pallas_call(
        functools.partial(project_kernel, G, R),
        out_shape=jax.ShapeDtypeStruct((rows, width), jnp.float32),
        in_specs=[pl.BlockSpec(memory_space=pltpu.VMEM)] * 4,
        out_specs=pl.BlockSpec(memory_space=pltpu.VMEM),
        scratch_shapes=[
            pltpu.VMEM((G, tok, feat), jnp.bfloat16),
            pltpu.VMEM((R - 1, 3, krows, col_width), jnp.bfloat16),
            pltpu.VMEM((pairs, 2, rows, width), jnp.bfloat16),
            pltpu.VMEM((G, rows, width), jnp.bfloat16),
            dma, dma, dma, dma((G - 1,)), dma((G - 1,)),
            dma((pairs, R - 1, 3)), dma((pairs, R - 1, 3)),
            dma((pairs, 2, G)), dma((G, G)),
        ],
        compiler_params=pltpu.CompilerParams(
            collective_id=0, has_side_effects=True, vmem_limit_bytes=58 * 2**20),
        cost_estimate=pl.CostEstimate(
            flops=2 * rows * feat * 3 * col_width, bytes_accessed=300 * 2**20, transcendentals=0),
    )(activity, wq, wk, wv)


def rotate(channels, angle_pos):
    half_width = channels.shape[-1] // 2
    frequency = rope_base ** (
        -jnp.arange(0, half_width, dtype=jnp.float32) * 2.0 / channels.shape[-1]
    )
    angles = angle_pos[:, :, None] * frequency
    cosine = jnp.cos(angles)[:, :, None, :]
    sine_part = jnp.sin(angles)[:, :, None, :]
    first_half = channels[..., :half_width]
    second_half = channels[..., half_width:]
    return jnp.concatenate(
        [
            first_half * cosine - second_half * sine_part,
            second_half * cosine + first_half * sine_part,
        ],
        axis=-1,
    )


def window_mix(queries, key_rows, value_rows, first_pos, dilation):
    blocks, tok, _ = queries.shape
    steps = tok // dilation
    kept = SPAN + steps
    q = queries.reshape(blocks, steps, dilation, HEAD)
    k = key_rows.reshape(blocks, kept, dilation, HEAD)
    v = value_rows.reshape(blocks, kept, dilation, HEAD)
    scores = jnp.einsum("zadc,zrdc->zdar", q, k, preferred_element_type=jnp.float32)
    scores = scores * HEAD ** (-0.5)
    step_gap = (
        SPAN
        + jnp.arange(steps, dtype=jnp.int32)[:, None]
        - jnp.arange(kept, dtype=jnp.int32)[None, :]
    )
    key_pos = (
        first_pos[:, None, None]
        + jnp.arange(kept, dtype=jnp.int32)[None, None, :] * dilation
        + jnp.arange(dilation, dtype=jnp.int32)[None, :, None]
    )
    allowed = ((step_gap >= 0) & (step_gap <= SPAN))[None, None] & (key_pos >= 0)[:, :, None, :]
    scores = jnp.where(allowed, scores, -jnp.inf)
    row_max = jnp.max(scores, axis=-1, keepdims=True)
    expo = jnp.where(allowed, jnp.exp(scores - row_max), 0.0)
    denominator = jnp.sum(expo, axis=-1)
    mixed = jnp.einsum(
        "zdar,zrdc->zadc", expo.astype(jnp.bfloat16), v, preferred_element_type=jnp.float32
    )
    mixed = mixed / jnp.transpose(denominator, (0, 2, 1))[..., None]
    log_total = jnp.transpose(row_max[..., 0] + jnp.log(denominator), (0, 2, 1))
    return mixed.reshape(blocks, tok, HEAD), log_total.reshape(blocks, tok)


def per_device(activity, query_weight, key_weight, value_weight, merge_weight):
    G = lax.axis_size("tp")
    R = lax.axis_size("sp") // G
    s = lax.axis_index("sp")
    r = s % R
    tok = activity.shape[0]
    total_tok = G * R * tok
    group_cols = HEAD_GROUPS * HEAD
    merge_full = lax.all_gather(merge_weight, "sp", axis=1, tiled=True)
    qkv = project(activity, query_weight, key_weight, value_weight, G, R)
    block_start = (jnp.arange(G, dtype=jnp.int32) * R + r) * tok
    pos = block_start[:, None] + jnp.arange(tok, dtype=jnp.int32)[None, :]
    qkv = qkv.reshape(G, tok, 3, HEAD_GROUPS, HEAD)
    turned = rotate(
        qkv[:, :, :2].reshape(G, tok, 2 * HEAD_GROUPS, HEAD), pos.astype(jnp.float32)
    ).astype(jnp.bfloat16)
    queries = turned[:, :, :HEAD_GROUPS]
    kv = jnp.concatenate(
        [
            turned[:, :, HEAD_GROUPS:].reshape(G, tok, group_cols),
            qkv[:, :, 2].astype(jnp.bfloat16).reshape(G, tok, group_cols),
        ],
        axis=-1,
    )
    held = [kv]
    for i in range(1, R):
        perm = [(a * R + b, a * R + (b - i) % R) for a in range(G) for b in range(R)]
        held.append(lax.ppermute(kv, "sp", perm))
    ordered = jnp.roll(jnp.stack(held), r, axis=0)
    kv_all = jnp.transpose(ordered, (1, 0, 2, 3)).reshape(total_tok, 2 * group_cols)
    most = SPAN * DILATIONS[-1]
    kv_all = jnp.pad(kv_all, ((most, 0), (0, 0)))
    windows = jnp.stack([
        lax.dynamic_slice_in_dim(kv_all, (a * R + r) * tok, most + tok, 0) for a in range(G)
    ])
    mixed_list = []
    total_list = []
    for index, dilation in enumerate(DILATIONS):
        reach = SPAN * dilation
        near = windows[:, most - reach:]
        keys = near[:, :, index * HEAD:(index + 1) * HEAD]
        values = near[:, :, group_cols + index * HEAD:group_cols + (index + 1) * HEAD]
        mixed, log_total = window_mix(
            queries[:, :, index], keys, values, block_start - reach, dilation)
        mixed_list.append(mixed)
        total_list.append(log_total)
    total_stack = jnp.stack(total_list)
    shifted = jnp.exp(total_stack - jnp.max(total_stack, axis=0))
    group_weight = shifted / jnp.sum(shifted, axis=0)
    merged = jnp.sum(group_weight[..., None] * jnp.stack(mixed_list), axis=0).astype(jnp.bfloat16)
    groups = [[a * R + b for a in range(G)] for b in range(R)]
    merged = lax.all_to_all(merged, "sp", 0, 0, axis_index_groups=groups)
    merged = jnp.transpose(merged, (1, 0, 2)).reshape(tok, G * HEAD)
    return lax.psum_scatter(
        jnp.dot(merged, merge_full, preferred_element_type=jnp.float32).astype(jnp.bfloat16),
        "tp",
        scatter_dimension=0,
        tiled=True,
    )


def solution(mesh):
    placed = (P("sp", "tp"), P("sp", "tp"), P("sp", "tp"), P("sp", "tp"), P("tp", "sp"))
    return jax.shard_map(
        per_device, mesh=mesh, in_specs=placed, out_specs=P(("sp", "tp"), None), check_vma=False
    )
```

```python
import functools

import jax
import jax.numpy as jnp
from jax import lax
from jax.experimental import pallas as pl
from jax.experimental.pallas import tpu as pltpu
from jax.sharding import PartitionSpec as P

HEAD = 64
HEAD_GROUPS = 3
SPAN = 128
DILATIONS = (1, 4, 8)
MESH = pl.DeviceIdType.MESH

rope_base = 500000.0


def project_kernel(
    G, R, act, wq, wk, wv, cos_ref, sin_ref, out,
    a_buf, w_buf, c_buf, r_buf, q_buf, kv_buf, o_buf, m_buf,
    local_sem, swap_send, swap_recv, fan_send, fan_recv,
    w_send, w_recv, c_send, c_recv, kv_send, kv_recv, m_send, m_recv,
):
    s = lax.axis_index("sp")
    t = lax.axis_index("tp")
    g = lax.div(s, R)
    r = lax.rem(s, R)
    tok = act.shape[0]
    krows = wq.shape[0]
    width = wq.shape[1] // G
    pairs = G // 2
    weights = (wq, wk, wv)

    swap_dev = (t * R + r, g)
    barrier = pltpu.get_barrier_semaphore()

    def greet(dev):
        pl.semaphore_signal(barrier, inc=1, device_id=dev, device_id_type=MESH)

    for i in range(1, G):
        greet((s, lax.rem(t + i, G)))
        greet((lax.rem(g + i, G) * R + r, t))
    for i in range(1, R):
        greet((g * R + lax.rem(r + i, R), t))

    @pl.when(g != t)
    def _():
        greet(swap_dev)

    pl.semaphore_wait(barrier, 2 * (G - 1) + (R - 1) + jnp.where(g != t, 1, 0))

    def swap_copy():
        return pltpu.make_async_remote_copy(
            src_ref=act, dst_ref=a_buf.at[g], send_sem=swap_send, recv_sem=swap_recv,
            device_id=swap_dev, device_id_type=MESH)

    def swap_local():
        return pltpu.make_async_copy(act, a_buf.at[t], local_sem)

    @pl.when(g != t)
    def _():
        swap_copy().start()

    @pl.when(g == t)
    def _():
        swap_local().start()

    def pair_at(stage):
        return lax.rem(lax.div(g, 2) + 1 + stage, pairs)

    def pair_cols(stage):
        return pl.ds(pl.multiple_of(pair_at(stage) * (2 * width), 128), 2 * width)

    def w_copy(stage, i, x):
        cols = pair_cols(stage)
        return pltpu.make_async_remote_copy(
            src_ref=weights[x].at[:, cols], dst_ref=w_buf.at[i - 1, x, :, cols],
            send_sem=w_send.at[stage, i - 1, x], recv_sem=w_recv.at[stage, i - 1, x],
            device_id=(g * R + lax.rem(r + R - i, R), t), device_id_type=MESH)

    for stage in range(pairs):
        for i in range(1, R):
            for x in range(3):
                w_copy(stage, i, x).start()

    @pl.when(g != t)
    def _():
        swap_copy().wait_recv()

    @pl.when(g == t)
    def _():
        swap_local().wait()

    def fan_copy(i):
        return pltpu.make_async_remote_copy(
            src_ref=a_buf.at[t], dst_ref=a_buf.at[t], send_sem=fan_send.at[i - 1],
            recv_sem=fan_recv.at[i - 1],
            device_id=(s, lax.rem(t + i, G)), device_id_type=MESH)

    def fan_arrival(i):
        slot = lax.rem(t + G - i, G)
        return pltpu.make_async_remote_copy(
            src_ref=a_buf.at[slot], dst_ref=a_buf.at[slot], send_sem=fan_send.at[i - 1],
            recv_sem=fan_recv.at[i - 1],
            device_id=(s, lax.rem(t + i, G)), device_id_type=MESH)

    for i in range(1, G):
        fan_copy(i).start()
    for i in range(1, G):
        fan_arrival(i).wait_recv()

    def c_copy(stage, j, b):
        dest = pair_at(stage) * 2 + j
        rows = pl.ds(pl.multiple_of(b * tok, tok), tok)
        return pltpu.make_async_remote_copy(
            src_ref=c_buf.at[stage, j, rows], dst_ref=r_buf.at[g, rows],
            send_sem=c_send.at[stage, j, b], recv_sem=c_recv.at[g, b],
            device_id=(dest * R + r, t), device_id_type=MESH)

    for stage in range(pairs):
        for i in range(1, R):
            for x in range(3):
                w_copy(stage, i, x).wait_recv()
        cols = pair_cols(stage)

        @pl.loop(0, G)
        def _(b):
            parts = []
            for x in range(3):
                total = jnp.dot(
                    a_buf[b, :, pl.ds(pl.multiple_of(r * krows, 128), krows)],
                    weights[x][:, cols], preferred_element_type=jnp.float32)
                for i in range(1, R):
                    start = pl.multiple_of(lax.rem(r + i, R) * krows, 128)
                    total = total + jnp.dot(
                        a_buf[b, :, pl.ds(start, krows)], w_buf[i - 1, x, :, cols],
                        preferred_element_type=jnp.float32)
                parts.append(total)
            rows = pl.ds(pl.multiple_of(b * tok, tok), tok)
            for j in range(2):
                c_buf[stage, j, rows, :] = jnp.concatenate(
                    [part[:, j * width:(j + 1) * width] for part in parts], axis=1
                ).astype(jnp.bfloat16)
            for j in range(2):
                @pl.when(pair_at(stage) * 2 + j != g)
                def _():
                    c_copy(stage, j, b).start()

    def c_arrival(source, b):
        rows = pl.ds(pl.multiple_of(b * tok, tok), tok)
        return pltpu.make_async_remote_copy(
            src_ref=r_buf.at[source, rows], dst_ref=r_buf.at[source, rows],
            send_sem=c_send.at[0, 0, b], recv_sem=c_recv.at[source, b],
            device_id=(s, t), device_id_type=MESH)

    mine = lax.rem(g, 2)
    most = SPAN * DILATIONS[-1]
    kv_buf[0:most, :] = jnp.zeros((most, 2 * width), jnp.bfloat16)

    def kv_rows(b, part):
        return pl.ds(pl.multiple_of(most + (b * R + part) * tok, 128), tok)

    def kv_copy(i, b):
        rows = kv_rows(b, r)
        return pltpu.make_async_remote_copy(
            src_ref=kv_buf.at[rows], dst_ref=kv_buf.at[rows],
            send_sem=kv_send.at[i - 1, b], recv_sem=kv_recv.at[i - 1, b],
            device_id=(g * R + lax.rem(r + R - i, R), t), device_id_type=MESH)

    def kv_arrival(i, b):
        rows = kv_rows(b, lax.rem(r + i, R))
        return pltpu.make_async_remote_copy(
            src_ref=kv_buf.at[rows], dst_ref=kv_buf.at[rows],
            send_sem=kv_send.at[i - 1, b], recv_sem=kv_recv.at[i - 1, b],
            device_id=(g * R + lax.rem(r + R - i, R), t), device_id_type=MESH)

    @pl.loop(0, G)
    def _(b):
        rows = pl.ds(pl.multiple_of(b * tok, tok), tok)
        total = c_buf[pairs - 1, mine, rows, :].astype(jnp.float32)
        for i in range(1, G):
            source = lax.rem(g + i, G)
            c_arrival(source, b).wait_recv()
            total = total + r_buf[source, rows, :].astype(jnp.float32)
        turn = total[:, :2 * width]
        half = HEAD // 2
        ahead = jnp.concatenate([turn[:, half:], turn[:, :half]], axis=1)
        behind = jnp.concatenate([turn[:, -half:], turn[:, :-half]], axis=1)
        lane = lax.broadcasted_iota(jnp.int32, turn.shape, 1)
        other = jnp.where((lane & (HEAD - 1)) < half, ahead, behind)
        reps = 2 * width // cos_ref.shape[1]
        cosine = jnp.concatenate([cos_ref[rows, :]] * reps, axis=1)
        sine = jnp.concatenate([sin_ref[rows, :]] * reps, axis=1)
        turned = turn * cosine + other * sine
        q_buf[rows, :] = turned[:, :width].astype(jnp.bfloat16)
        kv_buf[kv_rows(b, r), :] = jnp.concatenate(
            [turned[:, width:], total[:, 2 * width:]], axis=1).astype(jnp.bfloat16)
        for i in range(1, R):
            kv_copy(i, b).start()

    @pl.loop(0, G)
    def _(b):
        for i in range(1, R):
            kv_arrival(i, b).wait_recv()

    def m_copy(b):
        return pltpu.make_async_remote_copy(
            src_ref=o_buf.at[b], dst_ref=m_buf.at[g],
            send_sem=m_send.at[b], recv_sem=m_recv.at[g],
            device_id=(b * R + r, t), device_id_type=MESH)

    def m_arrival(source):
        return pltpu.make_async_remote_copy(
            src_ref=m_buf.at[source], dst_ref=m_buf.at[source],
            send_sem=m_send.at[source], recv_sem=m_recv.at[source],
            device_id=(source * R + r, t), device_id_type=MESH)

    @pl.loop(0, G)
    def _(b):
        rows = pl.ds(pl.multiple_of(b * tok, tok), tok)
        first = (b * R + r) * tok
        mixed_list = []
        total_list = []
        for index, dilation in enumerate(DILATIONS):
            reach = SPAN * dilation
            keys = reach + tok
            near = pl.ds(pl.multiple_of(most - reach + first, 128), keys)
            q = q_buf[rows, index * HEAD:(index + 1) * HEAD]
            k = kv_buf[near, index * HEAD:(index + 1) * HEAD]
            v = kv_buf[near, width + index * HEAD:width + (index + 1) * HEAD]
            scores = lax.dot_general(
                q, k, (((1,), (1,)), ((), ())), preferred_element_type=jnp.float32
            ) * HEAD ** (-0.5)
            col = lax.broadcasted_iota(jnp.int32, (tok, keys), 1)
            gap = reach + lax.broadcasted_iota(jnp.int32, (tok, keys), 0) - col
            allowed = (gap >= 0) & (gap <= reach) & (col >= reach - first)
            if dilation > 1:
                allowed = allowed & ((gap & (dilation - 1)) == 0)
            scores = jnp.where(allowed, scores, -jnp.inf)
            row_max = jnp.max(scores, axis=1, keepdims=True)
            expo = jnp.exp(scores - row_max)
            denominator = jnp.sum(expo, axis=1, keepdims=True)
            mixed = jnp.dot(expo.astype(jnp.bfloat16), v, preferred_element_type=jnp.float32)
            mixed_list.append(mixed / denominator)
            total_list.append(row_max + jnp.log(denominator))
        peak = jnp.maximum(jnp.maximum(total_list[0], total_list[1]), total_list[2])
        shifted = [jnp.exp(one - peak) for one in total_list]
        whole = shifted[0] + shifted[1] + shifted[2]
        merged = sum(a / whole * b_ for a, b_ in zip(shifted, mixed_list)).astype(jnp.bfloat16)

        @pl.when(b != g)
        def _():
            o_buf[b] = merged
            m_copy(b).start()

        @pl.when(b == g)
        def _():
            m_buf[b] = merged

    for i in range(1, G):
        m_arrival(lax.rem(g + i, G)).wait_recv()
    out[...] = jnp.concatenate(
        [m_buf[h].astype(jnp.float32) for h in range(G)], axis=1).astype(jnp.bfloat16)

    for i in range(1, G):
        m_copy(lax.rem(g + i, G)).wait_send()

    @pl.loop(0, G)
    def _(b):
        for i in range(1, R):
            kv_copy(i, b).wait_send()

    @pl.when(g != t)
    def _():
        swap_copy().wait_send()

    for i in range(1, G):
        fan_copy(i).wait_send()
    for stage in range(pairs):
        for i in range(1, R):
            for x in range(3):
                w_copy(stage, i, x).wait_send()
        for j in range(2):
            @pl.when(pair_at(stage) * 2 + j != g)
            def _():
                @pl.loop(0, G)
                def _(b):
                    c_copy(stage, j, b).wait_send()


def project(activity, wq, wk, wv, cosine, sine, G, R):
    tok, feat = activity.shape
    krows, col_width = wq.shape
    width = 3 * (col_width // G)
    pairs = G // 2
    rows = G * tok
    dma = pltpu.SemaphoreType.DMA
    return pl.pallas_call(
        functools.partial(project_kernel, G, R),
        out_shape=jax.ShapeDtypeStruct((tok, G * HEAD), jnp.bfloat16),
        in_specs=[pl.BlockSpec(memory_space=pltpu.VMEM)] * 6,
        out_specs=pl.BlockSpec(memory_space=pltpu.VMEM),
        scratch_shapes=[
            pltpu.VMEM((G, tok, feat), jnp.bfloat16),
            pltpu.VMEM((R - 1, 3, krows, col_width), jnp.bfloat16),
            pltpu.VMEM((pairs, 2, rows, width), jnp.bfloat16),
            pltpu.VMEM((G, rows, width), jnp.bfloat16),
            pltpu.VMEM((rows, width // 3), jnp.bfloat16),
            pltpu.VMEM((SPAN * DILATIONS[-1] + R * rows, 2 * (width // 3)), jnp.bfloat16),
            pltpu.VMEM((G, tok, HEAD), jnp.bfloat16),
            pltpu.VMEM((G, tok, HEAD), jnp.bfloat16),
            dma, dma, dma, dma((G - 1,)), dma((G - 1,)),
            dma((pairs, R - 1, 3)), dma((pairs, R - 1, 3)),
            dma((pairs, 2, G)), dma((G, G)),
            dma((R - 1, G)), dma((R - 1, G)), dma((G,)), dma((G,)),
        ],
        compiler_params=pltpu.CompilerParams(
            collective_id=0, has_side_effects=True, vmem_limit_bytes=58 * 2**20),
        cost_estimate=pl.CostEstimate(
            flops=2 * rows * feat * 3 * col_width, bytes_accessed=300 * 2**20, transcendentals=0),
    )(activity, wq, wk, wv, cosine, sine)


def finish_kernel(merged, weight, out, near_out, near_in, far_out, far_in, held,
                  near_send, near_recv, far_send, far_recv):
    s = lax.axis_index("sp")
    t = lax.axis_index("tp")
    chunks = near_out.shape[0]
    rows = out.shape[0]
    cols = weight.shape[1] // chunks
    low = lax.rem(t, 2)
    near = t + 1 - 2 * low
    far = lax.rem(t + 2, 4)
    across = lax.rem(near + 2, 4)

    barrier = pltpu.get_barrier_semaphore()
    for peer in (near, far):
        pl.semaphore_signal(barrier, inc=1, device_id=(s, peer), device_id_type=MESH)
    pl.semaphore_wait(barrier, 2)

    def near_copy(c):
        return pltpu.make_async_remote_copy(
            src_ref=near_out.at[c], dst_ref=near_in.at[c], send_sem=near_send.at[c],
            recv_sem=near_recv.at[c], device_id=(s, near), device_id_type=MESH)

    def far_copy(c):
        return pltpu.make_async_remote_copy(
            src_ref=far_out.at[c], dst_ref=far_in.at[c], send_sem=far_send.at[c],
            recv_sem=far_recv.at[c], device_id=(s, far), device_id_type=MESH)

    def part(owner, at):
        picked = merged[pl.ds(pl.multiple_of(owner * rows, rows), rows), :]
        return jnp.dot(picked, weight[:, at], preferred_element_type=jnp.float32)

    @pl.loop(0, chunks)
    def _(c):
        at = pl.ds(pl.multiple_of(c * cols, 128), cols)
        near_out[c, 0] = part(across, at).astype(jnp.bfloat16)
        near_out[c, 1] = part(near, at).astype(jnp.bfloat16)
        near_copy(c).start()
        held[c, 0] = part(far, at)
        held[c, 1] = part(t, at)

    @pl.loop(0, chunks)
    def _(c):
        near_copy(c).wait_recv()
        far_out[c] = (held[c, 0] + near_in[c, 0].astype(jnp.float32)).astype(jnp.bfloat16)
        far_copy(c).start()
        held[c, 1] = held[c, 1] + near_in[c, 1].astype(jnp.float32)

    @pl.loop(0, chunks)
    def _(c):
        at = pl.ds(pl.multiple_of(c * cols, 128), cols)
        far_copy(c).wait_recv()
        out[:, at] = (held[c, 1] + far_in[c].astype(jnp.float32)).astype(jnp.bfloat16)

    @pl.loop(0, chunks)
    def _(c):
        near_copy(c).wait_send()
        far_copy(c).wait_send()


def finish(merged, weight, chunks):
    rows = merged.shape[0] // 4
    cols = weight.shape[1] // chunks
    dma = pltpu.SemaphoreType.DMA
    return pl.pallas_call(
        finish_kernel,
        out_shape=jax.ShapeDtypeStruct((rows, weight.shape[1]), jnp.bfloat16),
        in_specs=[pl.BlockSpec(memory_space=pltpu.VMEM)] * 2,
        out_specs=pl.BlockSpec(memory_space=pltpu.VMEM),
        scratch_shapes=[
            pltpu.VMEM((chunks, 2, rows, cols), jnp.bfloat16),
            pltpu.VMEM((chunks, 2, rows, cols), jnp.bfloat16),
            pltpu.VMEM((chunks, rows, cols), jnp.bfloat16),
            pltpu.VMEM((chunks, rows, cols), jnp.bfloat16),
            pltpu.VMEM((chunks, 2, rows, cols), jnp.float32),
            dma((chunks,)), dma((chunks,)), dma((chunks,)), dma((chunks,)),
        ],
        compiler_params=pltpu.CompilerParams(
            collective_id=1, has_side_effects=True, vmem_limit_bytes=40 * 2**20),
    )(merged, weight)


def per_device(activity, query_weight, key_weight, value_weight, merge_weight):
    G = lax.axis_size("tp")
    R = lax.axis_size("sp") // G
    r = lax.axis_index("sp") % R
    tok = activity.shape[0]
    merge_full = lax.all_gather(merge_weight, "sp", axis=1, tiled=True)
    block_start = (jnp.arange(G, dtype=jnp.int32) * R + r) * tok
    pos = (block_start[:, None] + jnp.arange(tok, dtype=jnp.int32)[None, :]).reshape(G * tok)
    half = HEAD // 2
    frequency = rope_base ** (-jnp.arange(0, half, dtype=jnp.float32) * 2.0 / HEAD)
    angles = pos.astype(jnp.float32)[:, None] * frequency[None, :]
    cosine = jnp.tile(jnp.cos(angles), (1, 4))
    sine = jnp.sin(angles)
    sine = jnp.tile(jnp.concatenate([-sine, sine], axis=1), (1, 2))
    merged = project(activity, query_weight, key_weight, value_weight, cosine, sine, G, R)
    return finish(merged, merge_full, 8)


def solution(mesh):
    placed = (P("sp", "tp"), P("sp", "tp"), P("sp", "tp"), P("sp", "tp"), P("tp", "sp"))
    return jax.shard_map(
        per_device, mesh=mesh, in_specs=placed, out_specs=P(("sp", "tp"), None), check_vma=False
    )
```

```python
import functools

import jax
import jax.numpy as jnp
from jax import lax
from jax.experimental import pallas as pl
from jax.experimental.pallas import tpu as pltpu
from jax.sharding import PartitionSpec as P

HEAD = 64
HEAD_GROUPS = 3
SPAN = 128
DILATIONS = (1, 4, 8)
MESH = pl.DeviceIdType.MESH

rope_base = 500000.0


def project_kernel(
    G, R, act, wq, wk, wv, cos_ref, sin_ref, out,
    a_buf, w_buf, c_buf, r_buf, q_buf, kv_buf, o_buf, m_buf,
    local_sem, swap_send, swap_recv, fan_send, fan_recv,
    w_send, w_recv, c_send, c_recv, kv_send, kv_recv, m_send, m_recv,
):
    s = lax.axis_index("sp")
    t = lax.axis_index("tp")
    g = lax.div(s, R)
    r = lax.rem(s, R)
    tok = act.shape[0]
    krows = wq.shape[0]
    width = wq.shape[1] // G
    pairs = G // 2
    weights = (wq, wk, wv)

    swap_dev = (t * R + r, g)
    barrier = pltpu.get_barrier_semaphore()

    def greet(dev):
        pl.semaphore_signal(barrier, inc=1, device_id=dev, device_id_type=MESH)

    for i in range(1, G):
        greet((s, lax.rem(t + i, G)))
        greet((lax.rem(g + i, G) * R + r, t))
    for i in range(1, R):
        greet((g * R + lax.rem(r + i, R), t))

    @pl.when(g != t)
    def _():
        greet(swap_dev)

    pl.semaphore_wait(barrier, 2 * (G - 1) + (R - 1) + jnp.where(g != t, 1, 0))

    def swap_copy():
        return pltpu.make_async_remote_copy(
            src_ref=act, dst_ref=a_buf.at[g], send_sem=swap_send, recv_sem=swap_recv,
            device_id=swap_dev, device_id_type=MESH)

    def swap_local():
        return pltpu.make_async_copy(act, a_buf.at[t], local_sem)

    @pl.when(g != t)
    def _():
        swap_copy().start()

    @pl.when(g == t)
    def _():
        swap_local().start()

    def pair_at(stage):
        return lax.rem(lax.div(g, 2) + 1 + stage, pairs)

    def pair_cols(stage):
        return pl.ds(pl.multiple_of(pair_at(stage) * (2 * width), 128), 2 * width)

    def w_copy(stage, i, x):
        cols = pair_cols(stage)
        return pltpu.make_async_remote_copy(
            src_ref=weights[x].at[:, cols], dst_ref=w_buf.at[i - 1, x, :, cols],
            send_sem=w_send.at[stage, i - 1, x], recv_sem=w_recv.at[stage, i - 1, x],
            device_id=(g * R + lax.rem(r + R - i, R), t), device_id_type=MESH)

    for stage in range(pairs):
        for i in range(1, R):
            for x in range(3):
                w_copy(stage, i, x).start()

    @pl.when(g != t)
    def _():
        swap_copy().wait_recv()

    @pl.when(g == t)
    def _():
        swap_local().wait()

    def fan_copy(i):
        return pltpu.make_async_remote_copy(
            src_ref=a_buf.at[t], dst_ref=a_buf.at[t], send_sem=fan_send.at[i - 1],
            recv_sem=fan_recv.at[i - 1],
            device_id=(s, lax.rem(t + i, G)), device_id_type=MESH)

    def fan_arrival(i):
        slot = lax.rem(t + G - i, G)
        return pltpu.make_async_remote_copy(
            src_ref=a_buf.at[slot], dst_ref=a_buf.at[slot], send_sem=fan_send.at[i - 1],
            recv_sem=fan_recv.at[i - 1],
            device_id=(s, lax.rem(t + i, G)), device_id_type=MESH)

    for i in range(1, G):
        fan_copy(i).start()
    for i in range(1, G):
        fan_arrival(i).wait_recv()

    def c_copy(stage, j, b):
        dest = pair_at(stage) * 2 + j
        rows = pl.ds(pl.multiple_of(b * tok, tok), tok)
        return pltpu.make_async_remote_copy(
            src_ref=c_buf.at[stage, j, rows], dst_ref=r_buf.at[g, rows],
            send_sem=c_send.at[stage, j, b], recv_sem=c_recv.at[g, b],
            device_id=(dest * R + r, t), device_id_type=MESH)

    for stage in range(pairs):
        for i in range(1, R):
            for x in range(3):
                w_copy(stage, i, x).wait_recv()
        cols = pair_cols(stage)

        @pl.loop(0, G)
        def _(b):
            parts = []
            for x in range(3):
                total = jnp.dot(
                    a_buf[b, :, pl.ds(pl.multiple_of(r * krows, 128), krows)],
                    weights[x][:, cols], preferred_element_type=jnp.float32)
                for i in range(1, R):
                    start = pl.multiple_of(lax.rem(r + i, R) * krows, 128)
                    total = total + jnp.dot(
                        a_buf[b, :, pl.ds(start, krows)], w_buf[i - 1, x, :, cols],
                        preferred_element_type=jnp.float32)
                parts.append(total)
            rows = pl.ds(pl.multiple_of(b * tok, tok), tok)
            for j in range(2):
                c_buf[stage, j, rows, :] = jnp.concatenate(
                    [part[:, j * width:(j + 1) * width] for part in parts], axis=1
                ).astype(jnp.bfloat16)
            for j in range(2):
                @pl.when(pair_at(stage) * 2 + j != g)
                def _():
                    c_copy(stage, j, b).start()

    def c_arrival(source, b):
        rows = pl.ds(pl.multiple_of(b * tok, tok), tok)
        return pltpu.make_async_remote_copy(
            src_ref=r_buf.at[source, rows], dst_ref=r_buf.at[source, rows],
            send_sem=c_send.at[0, 0, b], recv_sem=c_recv.at[source, b],
            device_id=(s, t), device_id_type=MESH)

    mine = lax.rem(g, 2)
    most = SPAN * DILATIONS[-1]
    kv_buf[0:most, :] = jnp.zeros((most, 2 * width), jnp.bfloat16)

    def kv_rows(b, part):
        return pl.ds(pl.multiple_of(most + (b * R + part) * tok, 128), tok)

    def kv_copy(i, b):
        rows = kv_rows(b, r)
        return pltpu.make_async_remote_copy(
            src_ref=kv_buf.at[rows], dst_ref=kv_buf.at[rows],
            send_sem=kv_send.at[i - 1, b], recv_sem=kv_recv.at[i - 1, b],
            device_id=(g * R + lax.rem(r + R - i, R), t), device_id_type=MESH)

    def kv_arrival(i, b):
        rows = kv_rows(b, lax.rem(r + i, R))
        return pltpu.make_async_remote_copy(
            src_ref=kv_buf.at[rows], dst_ref=kv_buf.at[rows],
            send_sem=kv_send.at[i - 1, b], recv_sem=kv_recv.at[i - 1, b],
            device_id=(g * R + lax.rem(r + R - i, R), t), device_id_type=MESH)

    def gather_block(b):
        rows = pl.ds(pl.multiple_of(b * tok, tok), tok)
        total = c_buf[pairs - 1, mine, rows, :].astype(jnp.float32)
        for i in range(1, G):
            source = lax.rem(g + i, G)
            c_arrival(source, b).wait_recv()
            total = total + r_buf[source, rows, :].astype(jnp.float32)
        turn = total[:, :2 * width]
        half = HEAD // 2
        ahead = jnp.concatenate([turn[:, half:], turn[:, :half]], axis=1)
        behind = jnp.concatenate([turn[:, -half:], turn[:, :-half]], axis=1)
        lane = lax.broadcasted_iota(jnp.int32, turn.shape, 1)
        other = jnp.where((lane & (HEAD - 1)) < half, ahead, behind)
        reps = 2 * width // cos_ref.shape[1]
        cosine = jnp.concatenate([cos_ref[rows, :]] * reps, axis=1)
        sine = jnp.concatenate([sin_ref[rows, :]] * reps, axis=1)
        turned = turn * cosine + other * sine
        q_buf[rows, :] = turned[:, :width].astype(jnp.bfloat16)
        kv_buf[kv_rows(b, r), :] = jnp.concatenate(
            [turned[:, width:], total[:, 2 * width:]], axis=1).astype(jnp.bfloat16)
        for i in range(1, R):
            kv_copy(i, b).start()

    def m_copy(b):
        return pltpu.make_async_remote_copy(
            src_ref=o_buf.at[b], dst_ref=m_buf.at[g],
            send_sem=m_send.at[b], recv_sem=m_recv.at[g],
            device_id=(b * R + r, t), device_id_type=MESH)

    def m_arrival(source):
        return pltpu.make_async_remote_copy(
            src_ref=m_buf.at[source], dst_ref=m_buf.at[source],
            send_sem=m_send.at[source], recv_sem=m_recv.at[source],
            device_id=(source * R + r, t), device_id_type=MESH)

    def attend(b):
        for i in range(1, R):
            kv_arrival(i, b).wait_recv()
        rows = pl.ds(pl.multiple_of(b * tok, tok), tok)
        first = (b * R + r) * tok
        mixed_list = []
        total_list = []
        for index, dilation in enumerate(DILATIONS):
            reach = SPAN * dilation
            keys = reach + tok
            near = pl.ds(pl.multiple_of(most - reach + first, 128), keys)
            q = q_buf[rows, index * HEAD:(index + 1) * HEAD]
            k = kv_buf[near, index * HEAD:(index + 1) * HEAD]
            v = kv_buf[near, width + index * HEAD:width + (index + 1) * HEAD]
            scores = lax.dot_general(
                q, k, (((1,), (1,)), ((), ())), preferred_element_type=jnp.float32
            ) * HEAD ** (-0.5)
            col = lax.broadcasted_iota(jnp.int32, (tok, keys), 1)
            gap = reach + lax.broadcasted_iota(jnp.int32, (tok, keys), 0) - col
            allowed = (gap >= 0) & (gap <= reach) & (col >= reach - first)
            if dilation > 1:
                allowed = allowed & ((gap & (dilation - 1)) == 0)
            scores = jnp.where(allowed, scores, -jnp.inf)
            row_max = jnp.max(scores, axis=1, keepdims=True)
            expo = jnp.exp(scores - row_max)
            denominator = jnp.sum(expo, axis=1, keepdims=True)
            mixed = jnp.dot(expo.astype(jnp.bfloat16), v, preferred_element_type=jnp.float32)
            mixed_list.append(mixed / denominator)
            total_list.append(row_max + jnp.log(denominator))
        peak = jnp.maximum(jnp.maximum(total_list[0], total_list[1]), total_list[2])
        shifted = [jnp.exp(one - peak) for one in total_list]
        whole = shifted[0] + shifted[1] + shifted[2]
        merged = sum(a / whole * b_ for a, b_ in zip(shifted, mixed_list)).astype(jnp.bfloat16)

        @pl.when(b != g)
        def _():
            o_buf[b] = merged
            m_copy(b).start()

        @pl.when(b == g)
        def _():
            m_buf[b] = merged

    gather_block(0)

    @pl.loop(1, G)
    def _(b):
        gather_block(b)
        attend(b - 1)

    attend(G - 1)

    for i in range(1, G):
        m_arrival(lax.rem(g + i, G)).wait_recv()
    out[...] = jnp.concatenate(
        [m_buf[h].astype(jnp.float32) for h in range(G)], axis=1).astype(jnp.bfloat16)

    for i in range(1, G):
        m_copy(lax.rem(g + i, G)).wait_send()

    @pl.loop(0, G)
    def _(b):
        for i in range(1, R):
            kv_copy(i, b).wait_send()

    @pl.when(g != t)
    def _():
        swap_copy().wait_send()

    for i in range(1, G):
        fan_copy(i).wait_send()
    for stage in range(pairs):
        for i in range(1, R):
            for x in range(3):
                w_copy(stage, i, x).wait_send()
        for j in range(2):
            @pl.when(pair_at(stage) * 2 + j != g)
            def _():
                @pl.loop(0, G)
                def _(b):
                    c_copy(stage, j, b).wait_send()


def project(activity, wq, wk, wv, cosine, sine, G, R):
    tok, feat = activity.shape
    krows, col_width = wq.shape
    width = 3 * (col_width // G)
    pairs = G // 2
    rows = G * tok
    dma = pltpu.SemaphoreType.DMA
    return pl.pallas_call(
        functools.partial(project_kernel, G, R),
        out_shape=jax.ShapeDtypeStruct((tok, G * HEAD), jnp.bfloat16),
        in_specs=[pl.BlockSpec(memory_space=pltpu.VMEM)] * 6,
        out_specs=pl.BlockSpec(memory_space=pltpu.VMEM),
        scratch_shapes=[
            pltpu.VMEM((G, tok, feat), jnp.bfloat16),
            pltpu.VMEM((R - 1, 3, krows, col_width), jnp.bfloat16),
            pltpu.VMEM((pairs, 2, rows, width), jnp.bfloat16),
            pltpu.VMEM((G, rows, width), jnp.bfloat16),
            pltpu.VMEM((rows, width // 3), jnp.bfloat16),
            pltpu.VMEM((SPAN * DILATIONS[-1] + R * rows, 2 * (width // 3)), jnp.bfloat16),
            pltpu.VMEM((G, tok, HEAD), jnp.bfloat16),
            pltpu.VMEM((G, tok, HEAD), jnp.bfloat16),
            dma, dma, dma, dma((G - 1,)), dma((G - 1,)),
            dma((pairs, R - 1, 3)), dma((pairs, R - 1, 3)),
            dma((pairs, 2, G)), dma((G, G)),
            dma((R - 1, G)), dma((R - 1, G)), dma((G,)), dma((G,)),
        ],
        compiler_params=pltpu.CompilerParams(
            collective_id=0, has_side_effects=True, vmem_limit_bytes=58 * 2**20),
        cost_estimate=pl.CostEstimate(
            flops=2 * rows * feat * 3 * col_width, bytes_accessed=300 * 2**20, transcendentals=0),
    )(activity, wq, wk, wv, cosine, sine)


def finish_kernel(merged, weight, out, near_out, near_in, far_out, far_in, held,
                  near_send, near_recv, far_send, far_recv):
    s = lax.axis_index("sp")
    t = lax.axis_index("tp")
    chunks = near_out.shape[0]
    rows = out.shape[0]
    cols = weight.shape[1] // chunks
    low = lax.rem(t, 2)
    near = t + 1 - 2 * low
    far = lax.rem(t + 2, 4)
    across = lax.rem(near + 2, 4)

    barrier = pltpu.get_barrier_semaphore()
    for peer in (near, far):
        pl.semaphore_signal(barrier, inc=1, device_id=(s, peer), device_id_type=MESH)
    pl.semaphore_wait(barrier, 2)

    def near_copy(c):
        return pltpu.make_async_remote_copy(
            src_ref=near_out.at[c], dst_ref=near_in.at[c], send_sem=near_send.at[c],
            recv_sem=near_recv.at[c], device_id=(s, near), device_id_type=MESH)

    def far_copy(c):
        return pltpu.make_async_remote_copy(
            src_ref=far_out.at[c], dst_ref=far_in.at[c], send_sem=far_send.at[c],
            recv_sem=far_recv.at[c], device_id=(s, far), device_id_type=MESH)

    def part(owner, at):
        picked = merged[pl.ds(pl.multiple_of(owner * rows, rows), rows), :]
        return jnp.dot(picked, weight[:, at], preferred_element_type=jnp.float32)

    @pl.loop(0, chunks)
    def _(c):
        at = pl.ds(pl.multiple_of(c * cols, 128), cols)
        near_out[c, 0] = part(across, at).astype(jnp.bfloat16)
        near_out[c, 1] = part(near, at).astype(jnp.bfloat16)
        near_copy(c).start()
        held[c, 0] = part(far, at)
        held[c, 1] = part(t, at)

    @pl.loop(0, chunks)
    def _(c):
        near_copy(c).wait_recv()
        far_out[c] = (held[c, 0] + near_in[c, 0].astype(jnp.float32)).astype(jnp.bfloat16)
        far_copy(c).start()
        held[c, 1] = held[c, 1] + near_in[c, 1].astype(jnp.float32)

    @pl.loop(0, chunks)
    def _(c):
        at = pl.ds(pl.multiple_of(c * cols, 128), cols)
        far_copy(c).wait_recv()
        out[:, at] = (held[c, 1] + far_in[c].astype(jnp.float32)).astype(jnp.bfloat16)

    @pl.loop(0, chunks)
    def _(c):
        near_copy(c).wait_send()
        far_copy(c).wait_send()


def finish(merged, weight, chunks):
    rows = merged.shape[0] // 4
    cols = weight.shape[1] // chunks
    dma = pltpu.SemaphoreType.DMA
    return pl.pallas_call(
        finish_kernel,
        out_shape=jax.ShapeDtypeStruct((rows, weight.shape[1]), jnp.bfloat16),
        in_specs=[pl.BlockSpec(memory_space=pltpu.VMEM)] * 2,
        out_specs=pl.BlockSpec(memory_space=pltpu.VMEM),
        scratch_shapes=[
            pltpu.VMEM((chunks, 2, rows, cols), jnp.bfloat16),
            pltpu.VMEM((chunks, 2, rows, cols), jnp.bfloat16),
            pltpu.VMEM((chunks, rows, cols), jnp.bfloat16),
            pltpu.VMEM((chunks, rows, cols), jnp.bfloat16),
            pltpu.VMEM((chunks, 2, rows, cols), jnp.float32),
            dma((chunks,)), dma((chunks,)), dma((chunks,)), dma((chunks,)),
        ],
        compiler_params=pltpu.CompilerParams(
            collective_id=1, has_side_effects=True, vmem_limit_bytes=40 * 2**20),
    )(merged, weight)


def per_device(activity, query_weight, key_weight, value_weight, merge_weight):
    G = lax.axis_size("tp")
    R = lax.axis_size("sp") // G
    r = lax.axis_index("sp") % R
    tok = activity.shape[0]
    merge_full = lax.all_gather(merge_weight, "sp", axis=1, tiled=True)
    block_start = (jnp.arange(G, dtype=jnp.int32) * R + r) * tok
    pos = (block_start[:, None] + jnp.arange(tok, dtype=jnp.int32)[None, :]).reshape(G * tok)
    half = HEAD // 2
    frequency = rope_base ** (-jnp.arange(0, half, dtype=jnp.float32) * 2.0 / HEAD)
    angles = pos.astype(jnp.float32)[:, None] * frequency[None, :]
    cosine = jnp.tile(jnp.cos(angles), (1, 4))
    sine = jnp.sin(angles)
    sine = jnp.tile(jnp.concatenate([-sine, sine], axis=1), (1, 2))
    merged = project(activity, query_weight, key_weight, value_weight, cosine, sine, G, R)
    return finish(merged, merge_full, 8)


def solution(mesh):
    placed = (P("sp", "tp"), P("sp", "tp"), P("sp", "tp"), P("sp", "tp"), P("tp", "sp"))
    return jax.shard_map(
        per_device, mesh=mesh, in_specs=placed, out_specs=P(("sp", "tp"), None), check_vma=False
    )
```
